32 devices in a mesh: ep: 8 (over z, core), tp: 4 (over y, x).
Axes of the slice: x: 2, y: 2, z: 4, core: 2. Of those that a mesh axis runs over, the one named last changes fastest.
Arguments:
- value_in: bfloat16 [8192, 1536], P('ep', 'tp'), may hold values from -6 to 6
- gate_in: bfloat16 [8192, 1536], P('ep', 'tp'), may hold values from -9 to 9
- conv_kernel: float32 [31, 1536], P(None, 'tp'), may hold values from -40 to 40
- norm_gain: float32 [1536], replicated, may hold values from 0.1 to 1.9
- norm_shift: float32 [1536], replicated, may hold values from -3 to 3
- out_weight: bfloat16 [1536, 2048], P(None, 'tp'), may hold values from -0.15625 to 0.15625
- expert_input: bfloat16 [1536, 2048], P('ep'), may hold values from -6 to 6
- expert_gain: float32 [2048], replicated, may hold values from 0.1 to 1.9
- route_ids: int32 [1536, 4], P('ep'), may hold values from 0 to 7, all different within a row; in each aligned block of 192 rows (0 to 191, 192 to 383, ...) at most 120 rows name the same one
- route_weights: float32 [1536, 4], P('ep'), may hold values from 0.2 to 1
- gate_weight: bfloat16 [8, 2048, 2048], P('ep', None, 'tp'), may hold values from -0.375 to 0.375
- up_weight: bfloat16 [8, 2048, 2048], P('ep', None, 'tp'), may hold values from -0.375 to 0.375
- down_weight: bfloat16 [8, 2048, 2048], P('ep', None, 'tp'), may hold values from -0.01953125 to 0.01953125
Outputs:
- mixed_out: bfloat16 [8192, 2048], P('ep', 'tp')
- routed_out: bfloat16 [1536, 2048], P('ep', 'tp')
The draws below stay inside these ranges and needn't reach their ends.
Inputs may be any that keep to these rules, and one draw needn't show every extreme that they name: `route_ids`: each row names 4 different experts; among the rows of one index of ep (aligned blocks of 192 rows) no expert is named by more than 120 rows, and in some block one expert is named by exactly 120.
All inputs are finite; a program needn't handle non-finite values.
Results may differ from the reference program's by a relative error of at most 0.0071.
Values may be sent and summed in bfloat16 or wider, within the bound.
No kernel may reach another device: no remote copies, remote signals or barrier semaphores. Data moves between devices by JAX's collectives and lax.ppermute only.
A program may use at most 64 MiB of HBM per device.

```python
import math
import jax
import jax.numpy as jnp
import numpy as np
from jax import lax

D = 2048
CH = 1536
FF = 2048
KW = 31
TOPK = 4
TOK_B = 192
EXPERTS = 8
CAP = 120
LENGTH = 8192
TOKENS_B = 1536
N_EP = 8


def draw_conv_kernel(key, part):
    first_key, second_key = jax.random.split(jax.random.fold_in(key, 17), 2)
    channel = jnp.arange(CH, dtype=jnp.float32) / CH
    jitter = jax.random.uniform(second_key, (CH,), jnp.float32, 0.0, 1.0)
    entries = jnp.clip(jax.random.normal(first_key, (KW, CH), jnp.float32), -4.0, 4.0)
    scales = 10.0 ** channel * 2.0 ** jitter
    return (entries * scales[None, :] * KW ** (-0.5)).astype(jnp.float32)


def steps_of(rng, extent, pieces, smallest, top_value):
    def one(dim, blocks):
        draws = jax.random.uniform(jax.random.fold_in(jax.random.fold_in(rng, 6), dim), (blocks,), jnp.float32, smallest / len(pieces), top_value / len(pieces))
        return jnp.repeat(jnp.exp(draws), extent[dim] // blocks).reshape((-1,) + (1,) * (len(extent) - dim - 1))

    factor_of = one(*pieces[0])
    for cut in pieces[1:]:
        factor_of = factor_of * one(*cut)
    return factor_of


def assign_block(key, own, number, rows, number_of, top, bound, lean):
    sequence = jax.random.permutation(key, number_of)
    packed, common = portions_of(number_of, rows * top, bound, lean, True), portions_of(number_of, rows * top, bound, lean, False)
    places = jnp.arange(number_of)

    def named(tallies, turn):
        used = int((tallies > 0).sum())
        fixed = max(1, used // 4)
        passed = fixed + (places - fixed + turn * (used - fixed)) % max(1, number_of - fixed)
        return jnp.zeros((number_of,), jnp.int32).at[sequence[jnp.where(places < fixed, places, passed)]].set(jnp.asarray(tallies, jnp.int32))

    tallies = jnp.where(number % 4 == 0, named(packed, number // 4), named(common, number - number // 4 - 1))
    mixed = jax.random.permutation(jax.random.fold_in(own, 3), number_of)
    donor, receiver = mixed[0:number_of // 2 * 2:2], mixed[1:number_of // 2 * 2:2]
    margin = jnp.minimum(tallies[donor] - 1, bound - tallies[receiver]) // 2
    margin = jnp.where((donor == sequence[0]) | (receiver == sequence[0]) | (tallies[receiver] == 0), 0, jnp.maximum(margin, 0))
    passed = jax.random.randint(jax.random.fold_in(own, 4), (number_of // 2,), 0, 1 << 20) % (margin + 1)
    tallies = tallies.at[donor].add(-passed).at[receiver].add(passed)
    members = jnp.searchsorted(jnp.cumsum(tallies), jnp.arange(rows * top), side="right").astype(jnp.int32)
    grid = members.reshape(top, rows).T
    grid = grid[jax.random.permutation(jax.random.fold_in(own, 1), rows)]
    turn = jax.random.randint(jax.random.fold_in(own, 2), (rows, 1), 0, top)
    return jnp.take_along_axis(grid, (jnp.arange(top)[None, :] + turn) % top, axis=1)


def portions_of(amount, total, limit, skew, full):
    portions = [(1 << 20) // math.isqrt(rank ** skew) + 1 for rank in range(1, amount + 1)]
    largest = limit if full else min(limit, max(-(-total // amount), total * portions[0] // sum(portions)))
    least = 1 if total - largest >= amount - 1 else 0
    given, rest = [largest] + [least] * (amount - 1), total - largest - least * (amount - 1)
    while rest > 0:
        free = [i for i in range(1, amount) if given[i] < largest] or [i for i in range(1, amount) if given[i] < limit]
        pool, remaining = sum([portions[i] for i in free]), rest
        for i in free:
            extra = min(limit - given[i], max(1, remaining * portions[i] // pool), rest)
            given[i] = given[i] + extra
            rest = rest - extra
    return np.array(given)


def gaussian(own_key, shape, width, limit, cuts=(), kind=jnp.bfloat16):
    values = jax.random.normal(own_key, shape, jnp.float32) * width
    if len(cuts) > 0:
        values = steps_of(own_key, shape, cuts, -0.22, 0.18) * values
    return jnp.clip(values, min=-limit, max=limit).astype(kind)


def setup_inputs(seed: int = 0) -> dict:
    key_list = jax.random.split(jax.random.key(seed), 14)
    value_in = gaussian(key_list[0], (LENGTH, CH), 1.0, 6.0, ((0, 8), (1, 4)))
    gate_in = gaussian(key_list[1], (LENGTH, CH), 1.5, 9.0, ((0, 8), (1, 4)))
    conv_kernel = draw_conv_kernel(jax.random.fold_in(key_list[13], 71), 0)
    norm_gain = jnp.clip(1.0 + 0.18 * jax.random.normal(key_list[3], (CH,), jnp.float32), 0.1, 1.9)
    norm_shift = gaussian(key_list[4], (CH,), 0.5, 3.0, (), jnp.float32)
    out_weight = gaussian(key_list[5], (CH, D), CH ** -0.5, 0.15625, ((1, 4),))
    expert_input = gaussian(key_list[6], (TOKENS_B, D), 1.0, 6.0, ((0, 8),))
    expert_gain = jnp.clip(1.0 + 0.18 * jax.random.normal(key_list[7], (D,), jnp.float32), 0.1, 1.9)
    route_ids_keys = jax.random.split(jax.random.fold_in(key_list[8], 1), TOKENS_B // TOK_B)
    route_ids_turns = jax.random.permutation(jax.random.fold_in(key_list[8], 3), TOKENS_B // TOK_B)
    route_ids = jax.vmap(lambda own, number: assign_block(jax.random.fold_in(key_list[8], 2), own, number, TOK_B, EXPERTS, TOPK, CAP, 2))(route_ids_keys, route_ids_turns).reshape((TOKENS_B, TOPK))
    route_weights = jnp.clip(0.2 + 0.8 * jax.random.uniform(key_list[9], (TOKENS_B, TOPK), jnp.float32) ** steps_of(key_list[9], (TOKENS_B, TOPK), ((0, 8),), -0.2, 0.2), 0.2, 1.0)
    gate_weight = gaussian(key_list[10], (EXPERTS, D, FF), (D // 9) ** -0.5, 0.375, ((0, 8), (2, 4)))
    up_weight = gaussian(key_list[11], (EXPERTS, D, FF), (D // 9) ** -0.5, 0.375, ((0, 8), (2, 4)))
    down_weight = gaussian(key_list[12], (EXPERTS, FF, D), (45 * FF) ** -0.5, 0.01953125, ((0, 8), (2, 4)))
    return {"value_in": value_in, "gate_in": gate_in, "conv_kernel": conv_kernel, "norm_gain": norm_gain, "norm_shift": norm_shift, "out_weight": out_weight, "expert_input": expert_input, "expert_gain": expert_gain, "route_ids": route_ids, "route_weights": route_weights, "gate_weight": gate_weight, "up_weight": up_weight, "down_weight": down_weight}


def reference(value_in, gate_in, conv_kernel, norm_gain, norm_shift, out_weight, expert_input, expert_gain, route_ids, route_weights, gate_weight, up_weight, down_weight):
    gated_values = (value_in.astype(jnp.float32) * jax.nn.sigmoid(gate_in.astype(jnp.float32))).astype(jnp.bfloat16)
    kernel_width = conv_kernel.shape[0]
    positions = gated_values.shape[0]
    padded = jnp.concatenate([jnp.zeros((kernel_width - 1, gated_values.shape[1]), jnp.bfloat16), gated_values], 0)
    running = jnp.zeros(gated_values.shape, jnp.float32)
    for tap_index in range(kernel_width):
        running = running + conv_kernel[tap_index][None, :] * padded[tap_index:tap_index + positions].astype(jnp.float32)
    convolved = running.astype(jnp.bfloat16)
    conv_float = convolved.astype(jnp.float32)
    row_mean = lax.optimization_barrier(jnp.mean(conv_float, axis=1, keepdims=True))
    row_var = lax.optimization_barrier(jnp.mean(jnp.square(conv_float - row_mean), axis=1, keepdims=True))
    normed = (conv_float - row_mean) * lax.rsqrt(row_var + 1e-05) * norm_gain[None, :] + norm_shift[None, :]
    hidden = jax.nn.silu(normed).astype(jnp.bfloat16)
    mixed_out = jnp.dot(hidden, out_weight, preferred_element_type=jnp.float32).astype(jnp.bfloat16)
    input_float = expert_input.astype(jnp.float32)
    feature_mean = lax.optimization_barrier(jnp.mean(input_float, axis=1, keepdims=True))
    feature_var = lax.optimization_barrier(jnp.mean(jnp.square(input_float - feature_mean), axis=1, keepdims=True))
    normed_rows = ((input_float - feature_mean) * lax.rsqrt(feature_var + 1e-05) * expert_gain[None, :]).astype(jnp.bfloat16)
    row_total = expert_input.shape[0]
    block_ids = route_ids.reshape(N_EP, TOK_B * TOPK)
    onehot = (block_ids[:, :, None] == jnp.arange(EXPERTS, dtype=jnp.int32)[None, None, :]).astype(jnp.int32)
    earlier = jnp.cumsum(onehot, axis=1) - onehot
    position = lax.optimization_barrier(jnp.sum(earlier * onehot, axis=2))
    blocks = jnp.arange(N_EP, dtype=jnp.int32)[:, None]
    slot_index = (block_ids * (N_EP * CAP) + blocks * CAP + position).reshape(-1).astype(jnp.int32)
    token_index = jnp.arange(N_EP * TOK_B * TOPK, dtype=jnp.int32) // TOPK
    slot_table = jnp.full((EXPERTS * N_EP * CAP,), row_total, jnp.int32).at[slot_index].set(token_index)
    padded_rows = jnp.concatenate([normed_rows, jnp.zeros((1, normed_rows.shape[1]), jnp.bfloat16)], 0)

    def run_expert(operands):
        table_rows, gate_matrix, up_matrix, down_matrix = operands
        slot_rows = padded_rows[table_rows]
        gate_pre = jnp.dot(slot_rows, gate_matrix, preferred_element_type=jnp.float32)
        up_pre = jnp.dot(slot_rows, up_matrix, preferred_element_type=jnp.float32)
        clamped = jnp.minimum(gate_pre, 7.0)
        upward = jnp.clip(up_pre, -7.0, 7.0)
        activation = ((upward + 1.0) * clamped * jax.nn.sigmoid(1.702 * clamped)).astype(jnp.bfloat16)
        return jnp.dot(activation, down_matrix, preferred_element_type=jnp.float32).astype(jnp.bfloat16)
    results = lax.map(run_expert, (slot_table.reshape(EXPERTS, N_EP * CAP), gate_weight, up_weight, down_weight))
    picked = results.reshape(-1, results.shape[2])[slot_index].reshape(row_total, TOPK, -1).astype(jnp.float32)
    routed_out = lax.optimization_barrier(jnp.sum(picked * route_weights[:, :, None], axis=1)).astype(jnp.bfloat16)
    return (mixed_out, routed_out)
```

```python
import jax
import jax.numpy as jnp
from jax import lax
from jax.sharding import PartitionSpec as P


F32 = jnp.float32
BF16 = jnp.bfloat16


def shifted(block, axis, distance):
    devices = range(lax.axis_size(axis))
    route = [(i - distance, i) for i in devices if i - distance in devices]
    return lax.ppermute(block, axis, route)


def swapped(block, axis, mask):
    return lax.ppermute(block, axis, [(i, i ^ mask) for i in range(lax.axis_size(axis))])


def gather_tp(block):
    near = swapped(block, "tp", 1)
    far = swapped(block, "tp", 2)
    half = block.shape[0] // 32 * 16
    top = swapped(near[:half], "tp", 2)
    bottom = swapped(far[half:], "tp", 1)
    return [block, near, far, jnp.concatenate([top, bottom], 0)]


def pieces_of(array, count, axis):
    width = array.shape[axis] // count
    own = lax.axis_index("tp")
    return [lax.dynamic_slice_in_dim(array, (own ^ k) * width, width, axis) for k in range(count)]


def relay_line(rows):
    z = lax.axis_index("ep") // 2

    def send(block, route):
        return lax.ppermute(block, "ep", [(a * 2 + c, b * 2 + c) for a, b in route for c in (0, 1)])

    below = send(rows, [(0, 1), (1, 2), (2, 3)])
    above = send(rows, [(1, 0), (2, 1), (3, 2)])
    second = send(below, [(1, 2), (2, 3)]) + send(above, [(1, 0), (2, 1)])
    third = send(second, [(1, 0), (2, 3)])
    odd = z % 2 == 1
    middle = (z == 1) | (z == 2)
    return [
        jnp.where(odd, below, above),
        second,
        jnp.where(middle, jnp.where(odd, above, below), third),
    ]


def activate(gate_pre, up_pre):
    clamped = jnp.minimum(gate_pre, 7.0)
    upward = jnp.clip(up_pre, -7.0, 7.0)
    return ((upward + 1.0) * clamped * jax.nn.sigmoid(1.702 * clamped)).astype(BF16)


def dot(a, b):
    return jnp.dot(a, b, preferred_element_type=F32)


def body(
    value_in,
    gate_in,
    conv_kernel,
    norm_gain,
    norm_shift,
    out_weight,
    expert_input,
    expert_gain,
    route_ids,
    route_weights,
    gate_weight,
    up_weight,
    down_weight,
):
    experts = lax.axis_size("ep")
    tensor = lax.axis_size("tp")
    chips = experts // 2
    chunked = chips == 4 and tensor == 4
    me = lax.axis_index("ep")
    row_count, model_width = expert_input.shape
    top_count = route_ids.shape[1]
    capacity = (5 * row_count * top_count + 4 * experts - 1) // (4 * experts)

    input_float = expert_input.astype(F32)
    feature_mean = jnp.mean(input_float, axis=1, keepdims=True)
    feature_var = jnp.mean(jnp.square(input_float - feature_mean), axis=1, keepdims=True)
    normed_rows = (
        (input_float - feature_mean) * lax.rsqrt(feature_var + 1e-05) * expert_gain[None, :]
    ).astype(BF16)
    ids_all = lax.all_gather(route_ids, "ep", axis=0)
    if chunked:
        remote = relay_line(normed_rows)
        own_side = [normed_rows] + remote
        chip_rows = [(block, swapped(block, "ep", 1)) for block in own_side]
        order = me ^ jnp.arange(experts, dtype=jnp.int32)
        chosen = order[:, None] == jnp.arange(experts, dtype=jnp.int32)[None, :]
        ids_of = jnp.sum(jnp.where(chosen[:, :, None, None], ids_all[None], 0), axis=1)
    else:
        order = jnp.arange(experts, dtype=jnp.int32)
        ids_of = ids_all

    row_index = jnp.arange(row_count, dtype=jnp.int32)
    before_row = (row_index[:, None] < row_index[None, :]).astype(BF16)
    slot_index = jnp.arange(capacity, dtype=jnp.int32)
    matched = jnp.any(ids_of == me, axis=2)
    position = dot(matched.astype(BF16), before_row).astype(jnp.int32)
    place = jnp.where(matched, position, -1)
    picker = (place[:, None, :] == slot_index[None, :, None]).astype(BF16)
    named = route_ids[None, :, :] == order[:, None, None]
    mine = jnp.any(named, axis=2)
    weight_of = jnp.sum(jnp.where(named, route_weights[None], 0.0), axis=2)
    home = dot(mine.astype(BF16), before_row).astype(jnp.int32)
    home = jnp.where(mine, home, -1)
    spread = jnp.where(home[:, :, None] == slot_index[None, None, :], weight_of[:, :, None], 0.0)
    spread_high = spread.astype(BF16)
    spread_low = (spread - spread_high.astype(F32)).astype(BF16)
    spread_both = jnp.concatenate([spread_high, spread_low], 1)

    gated_values = (value_in.astype(F32) * jax.nn.sigmoid(gate_in.astype(F32))).astype(BF16)
    kernel_width = conv_kernel.shape[0]
    length_dev, channels_dev = gated_values.shape
    before = shifted(gated_values[length_dev - (kernel_width - 1) :], "ep", 1)
    extended = jnp.concatenate([before, gated_values], 0).astype(F32)
    running = jnp.zeros(gated_values.shape, F32)
    for tap_index in range(kernel_width):
        running = (
            running + conv_kernel[tap_index][None, :] * extended[tap_index : tap_index + length_dev]
        )
    convolved = running.astype(BF16)
    if chunked:
        parts = gather_tp(convolved)
        gains = pieces_of(norm_gain, tensor, 0)
        shifts = pieces_of(norm_shift, tensor, 0)
        outs = pieces_of(out_weight, tensor, 0)
    else:
        parts = [lax.all_gather(convolved, "tp", axis=1, tiled=True)]
        gains, shifts, outs = [norm_gain], [norm_shift], [out_weight]
    channels = norm_gain.shape[0]
    row_mean = sum(jnp.sum(p.astype(F32), axis=1, keepdims=True) for p in parts) / channels
    row_var = (
        sum(jnp.sum(jnp.square(p.astype(F32) - row_mean), axis=1, keepdims=True) for p in parts)
        / channels
    )
    scale = lax.rsqrt(row_var + 1e-05)
    hidden = [
        jax.nn.silu((p.astype(F32) - row_mean) * scale * g[None, :] + s[None, :]).astype(BF16)
        for p, g, s in zip(parts, gains, shifts)
    ]
    mixed_out = dot(jnp.concatenate(hidden, 1), jnp.concatenate(outs, 0)).astype(BF16)

    gate_part, up_part = gate_weight[0], up_weight[0]
    if chunked:
        down_part = jnp.concatenate(pieces_of(down_weight[0], tensor, 0), 0)
        routed = jnp.zeros((2 * row_count, down_part.shape[1]), F32)
        for step, (same, cross) in enumerate(chip_rows):
            slots = jnp.concatenate(
                [dot(picker[2 * step], same), dot(picker[2 * step + 1], cross)], 0
            ).astype(BF16)
            activation = activate(dot(slots, gate_part), dot(slots, up_part))
            outcome = dot(jnp.concatenate(gather_tp(activation), 1), down_part).astype(BF16)
            for core in range(2):
                number = 2 * step + core
                back = outcome[core * capacity : (core + 1) * capacity]
                if number:
                    back = swapped(back, "ep", number)
                routed = routed + dot(spread_both[number], back)
    else:
        rows_all = lax.all_gather(normed_rows, "ep", axis=0)
        slots = jnp.einsum("bsr,brd->bsd", picker, rows_all, preferred_element_type=F32)
        slots = slots.astype(BF16).reshape(experts * capacity, model_width)
        activation = activate(dot(slots, gate_part), dot(slots, up_part))
        wide = lax.all_gather(activation, "tp", axis=1, tiled=True)
        outcome = dot(wide, down_weight[0]).astype(BF16)
        outcome = outcome.reshape(experts, capacity, outcome.shape[1])
        outcome = lax.all_to_all(outcome, "ep", split_axis=0, concat_axis=0, tiled=True)
        routed = jnp.einsum("ers,esd->rd", spread_both, outcome, preferred_element_type=F32)
    routed_out = (routed[:row_count] + routed[row_count:]).astype(BF16)
    return (mixed_out, routed_out)


def solution(mesh):
    return jax.shard_map(
        body,
        mesh=mesh,
        in_specs=(
            P("ep", "tp"),
            P("ep", "tp"),
            P(None, "tp"),
            P(),
            P(),
            P(None, "tp"),
            P("ep", None),
            P(),
            P("ep", None),
            P("ep", None),
            P("ep", None, "tp"),
            P("ep", None, "tp"),
            P("ep", None, "tp"),
        ),
        out_specs=(P("ep", "tp"), P("ep", "tp")),
        check_vma=False,
    )
```

```python
import jax
import jax.numpy as jnp
from jax import lax
from jax.sharding import PartitionSpec as P


F32 = jnp.float32
BF16 = jnp.bfloat16

CHUNKS = ((0, 1), (2,), (3,))


def shifted(block, axis, distance):
    devices = range(lax.axis_size(axis))
    route = [(i - distance, i) for i in devices if i - distance in devices]
    return lax.ppermute(block, axis, route)


def swapped(block, axis, mask):
    return lax.ppermute(block, axis, [(i, i ^ mask) for i in range(lax.axis_size(axis))])


def gather_tp(block):
    near = swapped(block, "tp", 1)
    far = swapped(block, "tp", 2)
    half = block.shape[0] // 32 * 16
    top = swapped(near[:half], "tp", 2)
    bottom = swapped(far[half:], "tp", 1)
    return [block, near, far, jnp.concatenate([top, bottom], 0)]


def pieces_of(array, count, axis):
    width = array.shape[axis] // count
    own = lax.axis_index("tp")
    return [lax.dynamic_slice_in_dim(array, (own ^ k) * width, width, axis) for k in range(count)]


def relay_line(rows):
    chips = lax.axis_size("ep") // 2
    z = lax.axis_index("ep") // 2

    def send(block, route):
        pairs = [(a * 2 + c, b * 2 + c) for a, b in route for c in (0, 1)]
        return lax.ppermute(block, "ep", pairs)

    below = send(rows, [(0, 1), (1, 2), (2, 3)])
    above = send(rows, [(1, 0), (2, 1), (3, 2)])
    far_below = send(below, [(1, 2), (2, 3)])
    far_above = send(above, [(1, 0), (2, 1)])
    last_below = send(far_below, [(2, 3)])
    last_above = send(far_above, [(1, 0)])
    odd = z % 2 == 1
    first, below, above = lax.optimization_barrier((jnp.where(odd, below, above), below, above))
    second = lax.optimization_barrier(jnp.where(z < 2, far_above, far_below))
    ends = jnp.where(z == 0, last_above, last_below)
    third = jnp.where((z == 0) | (z == chips - 1), ends, jnp.where(odd, above, below))
    return [first, second, third]


def activate(gate_pre, up_pre):
    clamped = jnp.minimum(gate_pre, 7.0)
    upward = jnp.clip(up_pre, -7.0, 7.0)
    return ((upward + 1.0) * clamped * jax.nn.sigmoid(1.702 * clamped)).astype(BF16)


def dot(a, b):
    return jnp.dot(a, b, preferred_element_type=F32)


def body(
    value_in,
    gate_in,
    conv_kernel,
    norm_gain,
    norm_shift,
    out_weight,
    expert_input,
    expert_gain,
    route_ids,
    route_weights,
    gate_weight,
    up_weight,
    down_weight,
):
    experts = lax.axis_size("ep")
    tensor = lax.axis_size("tp")
    chips = experts // 2
    chunked = chips == 4 and tensor == 4
    me = lax.axis_index("ep")
    row_count, model_width = expert_input.shape
    top_count = route_ids.shape[1]
    capacity = (5 * row_count * top_count + 4 * experts - 1) // (4 * experts)

    input_float = expert_input.astype(F32)
    feature_mean = jnp.mean(input_float, axis=1, keepdims=True)
    feature_var = jnp.mean(jnp.square(input_float - feature_mean), axis=1, keepdims=True)
    normed_rows = (
        (input_float - feature_mean) * lax.rsqrt(feature_var + 1e-05) * expert_gain[None, :]
    ).astype(BF16)
    tags = jnp.pad(route_ids.astype(BF16), ((0, 0), (0, 128 - top_count)))
    tagged = jnp.concatenate([normed_rows, tags], 1)
    if chunked:
        own_side = [tagged] + relay_line(tagged)
        chip_rows = [(block, swapped(block, "ep", 1)) for block in own_side]
        order = me ^ jnp.arange(experts, dtype=jnp.int32)
    else:
        order = jnp.arange(experts, dtype=jnp.int32)

    row_index = jnp.arange(row_count, dtype=jnp.int32)
    before_row = (row_index[:, None] < row_index[None, :]).astype(BF16)
    slot_index = jnp.arange(capacity, dtype=jnp.int32)

    def slots_of(blocks):
        names = blocks[:, :, model_width : model_width + top_count].astype(jnp.int32)
        matched = jnp.any(names == me, axis=2)
        position = dot(matched.astype(BF16), before_row).astype(jnp.int32)
        place = jnp.where(matched, position, -1)
        picker = (place[:, None, :] == slot_index[None, :, None]).astype(BF16)
        slots = jnp.einsum(
            "bsr,brd->bsd", picker, blocks[:, :, :model_width], preferred_element_type=F32
        )
        return slots.astype(BF16).reshape(-1, model_width)

    named = route_ids[None, :, :] == order[:, None, None]
    mine = jnp.any(named, axis=2)
    weight_of = jnp.sum(jnp.where(named, route_weights[None], 0.0), axis=2)
    home = dot(mine.astype(BF16), before_row).astype(jnp.int32)
    home = jnp.where(mine, home, -1)
    spread = jnp.where(home[:, :, None] == slot_index[None, None, :], weight_of[:, :, None], 0.0)
    spread_high = spread.astype(BF16)
    spread_low = (spread - spread_high.astype(F32)).astype(BF16)
    spread_both = jnp.concatenate([spread_high, spread_low], 1)

    gated_values = (value_in.astype(F32) * jax.nn.sigmoid(gate_in.astype(F32))).astype(BF16)
    kernel_width = conv_kernel.shape[0]
    length_dev, _ = gated_values.shape
    before = shifted(gated_values[length_dev - (kernel_width - 1) :], "ep", 1)
    extended = jnp.concatenate([before, gated_values], 0).astype(F32)
    running = jnp.zeros(gated_values.shape, F32)
    for tap_index in range(kernel_width):
        running = (
            running + conv_kernel[tap_index][None, :] * extended[tap_index : tap_index + length_dev]
        )
    convolved = running.astype(BF16)
    convolved, out_weight, down_weight = lax.optimization_barrier(
        (convolved, out_weight, down_weight)
    )
    if chunked:
        parts = gather_tp(convolved)
        gains = pieces_of(norm_gain, tensor, 0)
        shifts = pieces_of(norm_shift, tensor, 0)
        outs = pieces_of(out_weight, tensor, 0)
    else:
        parts = [lax.all_gather(convolved, "tp", axis=1, tiled=True)]
        gains, shifts, outs = [norm_gain], [norm_shift], [out_weight]
    channels = norm_gain.shape[0]
    row_mean = sum(jnp.sum(p.astype(F32), axis=1, keepdims=True) for p in parts) / channels
    row_var = (
        sum(jnp.sum(jnp.square(p.astype(F32) - row_mean), axis=1, keepdims=True) for p in parts)
        / channels
    )
    scale = lax.rsqrt(row_var + 1e-05)
    hidden = [
        jax.nn.silu((p.astype(F32) - row_mean) * scale * g[None, :] + s[None, :]).astype(BF16)
        for p, g, s in zip(parts, gains, shifts)
    ]
    mixed_out = dot(jnp.concatenate(hidden, 1), jnp.concatenate(outs, 0)).astype(BF16)

    gate_part, up_part = gate_weight[0], up_weight[0]
    if chunked:
        down_part = jnp.concatenate(pieces_of(down_weight[0], tensor, 0), 0)
        routed = jnp.zeros((2 * row_count, down_part.shape[1]), F32)
        for steps in CHUNKS:
            blocks = jnp.stack([block for step in steps for block in chip_rows[step]], 0)
            slots = slots_of(blocks)
            activation = activate(dot(slots, gate_part), dot(slots, up_part))
            wide = jnp.concatenate(gather_tp(activation), 1)
            outcome = dot(wide, down_part).astype(BF16)
            for place, expert in enumerate(2 * step + core for step in steps for core in range(2)):
                back = outcome[place * capacity : (place + 1) * capacity]
                if expert:
                    back = swapped(back, "ep", expert)
                routed = routed + dot(spread_both[expert], back)
    else:
        slots = slots_of(lax.all_gather(tagged, "ep", axis=0))
        activation = activate(dot(slots, gate_part), dot(slots, up_part))
        wide = lax.all_gather(activation, "tp", axis=1, tiled=True)
        outcome = dot(wide, down_weight[0]).astype(BF16)
        outcome = outcome.reshape(experts, capacity, outcome.shape[1])
        outcome = lax.all_to_all(outcome, "ep", split_axis=0, concat_axis=0, tiled=True)
        routed = jnp.einsum("ers,esd->rd", spread_both, outcome, preferred_element_type=F32)
    routed_out = (routed[:row_count] + routed[row_count:]).astype(BF16)
    return (mixed_out, routed_out)


def solution(mesh):
    return jax.shard_map(
        body,
        mesh=mesh,
        in_specs=(
            P("ep", "tp"),
            P("ep", "tp"),
            P(None, "tp"),
            P(),
            P(),
            P(None, "tp"),
            P("ep", None),
            P(),
            P("ep", None),
            P("ep", None),
            P("ep", None, "tp"),
            P("ep", None, "tp"),
            P("ep", None, "tp"),
        ),
        out_specs=(P("ep", "tp"), P("ep", "tp")),
        check_vma=False,
    )
```
